32 devices in a mesh: sp: 16 (over z, y, core), tp: 2 (over x).
Axes of the slice: x: 2, y: 2, z: 4, core: 2. Of those that a mesh axis runs over, the one named last changes fastest.
Arguments:
- tokens: bfloat16 [12288, 2048], P(('sp', 'tp')), may hold values from -6 to 6
- norm_gain: float32 [2048], replicated, may hold values from 0.1 to 1.9
- query_weight: bfloat16 [2048, 512], P(None, 'tp'), may hold values from -4 to 4
- key_weight: bfloat16 [2048, 256], P(None, 'tp'), may hold values from -4 to 4
- value_weight: bfloat16 [2048, 256], P(None, 'tp'), may hold values from -1 to 1
- sink_logit: float32 [8], P('tp'), may hold values from 2 to 6
- conv_gate_weight: bfloat16 [2048, 512], P(None, 'tp'), may hold values from -0.125 to 0.125
- conv_pre_weight: bfloat16 [2048, 512], P(None, 'tp'), may hold values from -0.125 to 0.125
- conv_input_weight: bfloat16 [2048, 512], P(None, 'tp'), may hold values from -0.125 to 0.125
- conv_taps: float32 [3, 512], P(None, 'tp'), may hold values from -3.5 to 3.5
- out_weight: bfloat16 [1024, 2048], replicated, may hold values from -0.1875 to 0.1875
Outputs:
- mixed: bfloat16 [12288, 2048], P(('sp', 'tp'))
The draws below stay inside these ranges and needn't reach their ends.
All inputs are finite; a program needn't handle non-finite values.
Results may differ from the reference program's by a relative error of at most 0.009.
Values may be sent and summed in bfloat16 or wider, within the bound.
A program may use at most 64 MiB of HBM per device.

```python
import jax
import jax.numpy as jnp
from jax import lax

D = 2048
QH = 8
KVH = 4
HEAD_SIZE = 64
CW = 512
WIN = 128
TOK_DEV = 768
TOKENS = 12288
N_SP = 16


def draw_pair(key):
    base = jax.random.fold_in(key, 11)
    key_part = jax.random.normal(jax.random.fold_in(base, 1), (D, KVH * HEAD_SIZE), jnp.float32) * D ** (-0.5)
    noise_part = jax.random.normal(jax.random.fold_in(base, 2), (D, QH * HEAD_SIZE), jnp.float32) * D ** (-0.5)
    query_part = noise_part
    return (jnp.clip(query_part, -4.0, 4.0), jnp.clip(key_part, -4.0, 4.0))


def draw_query_weight(key, part):
    return draw_pair(key)[0].astype(jnp.bfloat16)


def draw_key_weight(key, part):
    return draw_pair(key)[1].astype(jnp.bfloat16)


def level_of(rng, extent, split, low, high):
    factor_of, own = 1.0, jax.random.fold_in(rng, 6)
    for position, blocks in split:
        draws = jnp.exp(jax.random.uniform(jax.random.fold_in(own, position), (blocks,), jnp.float32, low / len(split), high / len(split)))
        factor_of = factor_of * jnp.repeat(draws, extent[position] // blocks).reshape([-1 if axis == position else 1 for axis in range(len(extent))])
    return factor_of


def scatter_about(stream_key, extent, deviation, limit, split=(), held_as=jnp.bfloat16):
    array = deviation * jax.random.normal(stream_key, extent, jnp.float32)
    if split:
        array = array * level_of(stream_key, extent, split, -0.22, 0.18)
    return jnp.clip(array, -limit, limit).astype(held_as)


def setup_inputs(seed: int = 0) -> dict:
    key_list = jax.random.split(jax.random.key(seed), 12)
    return {
        "tokens": scatter_about(key_list[0], (TOKENS, D), 1.0, 6.0, ((0, 32),)),
        "norm_gain": jnp.clip(1.0 + 0.18 * jax.random.normal(key_list[1], (D,), jnp.float32), 0.1, 1.9),
        "query_weight": draw_query_weight(jax.random.fold_in(key_list[11], 71), 0),
        "key_weight": draw_key_weight(jax.random.fold_in(key_list[11], 71), 0),
        "value_weight": scatter_about(key_list[4], (D, KVH * HEAD_SIZE), (D // 64) ** -0.5, 1.0, ((1, 2),)),
        "sink_logit": jnp.clip(2.0 + 4.0 * jax.random.uniform(key_list[5], (QH,), jnp.float32) ** level_of(key_list[5], (QH,), ((0, 2),), -0.2, 0.2), 2.0, 6.0),
        "conv_gate_weight": scatter_about(key_list[6], (D, CW), D ** -0.5, 0.125, ((1, 2),)),
        "conv_pre_weight": scatter_about(key_list[7], (D, CW), D ** -0.5, 0.125, ((1, 2),)),
        "conv_input_weight": scatter_about(key_list[8], (D, CW), D ** -0.5, 0.125, ((1, 2),)),
        "conv_taps": scatter_about(key_list[9], (3, CW), 3 ** -0.5, 3.5, ((1, 2),), jnp.float32),
        "out_weight": scatter_about(key_list[10], (QH * HEAD_SIZE + CW, D), (QH * HEAD_SIZE + CW) ** -0.5, 0.1875),
    }


def attend_block(query_block_tile, key_block_tile, value_block_tile, start, sinks, total):
    count = query_block_tile.shape[0]
    span = key_block_tile.shape[0]
    score_matrix = jnp.einsum('yxpz,ixz->xpyi', query_block_tile.astype(jnp.float32), key_block_tile.astype(jnp.float32)) * HEAD_SIZE ** (-0.5)
    query_pos = start + jnp.arange(count, dtype=jnp.int32)
    key_pos = start - WIN + jnp.arange(span, dtype=jnp.int32)
    valid = (jnp.abs(query_pos[:, None] - key_pos[None, :]) <= WIN) & (key_pos[None, :] >= 0) & (key_pos[None, :] < total)
    score_matrix = jnp.where(valid[None, None], score_matrix, -jnp.inf)
    sink_col = sinks.astype(jnp.float32)[:, :, None, None]
    top = jnp.maximum(lax.optimization_barrier(jnp.max(score_matrix, axis=-1, keepdims=True)), sink_col)
    expo = jnp.exp(score_matrix - top)
    denom = lax.optimization_barrier(jnp.sum(expo, axis=-1, keepdims=True)) + jnp.exp(sink_col - top)
    weight_lower_precision = (expo / denom).astype(jnp.bfloat16)
    final_output = jnp.einsum('bhcv,vbn->cbhn', weight_lower_precision.astype(jnp.float32), value_block_tile.astype(jnp.float32))
    return final_output.reshape(count, -1).astype(jnp.bfloat16)

def reference(tokens, norm_gain, query_weight, key_weight, value_weight, sink_logit, conv_gate_weight, conv_pre_weight, conv_input_weight, conv_taps, out_weight):
    tokens_f = tokens.astype(jnp.float32)
    normed = (tokens_f * lax.rsqrt(lax.optimization_barrier(jnp.mean(tokens_f * tokens_f, axis=-1, keepdims=True)) + 1e-06) * norm_gain).astype(jnp.bfloat16)
    queries = jnp.dot(normed, query_weight, preferred_element_type=jnp.float32).astype(jnp.bfloat16)
    key_rows = jnp.dot(normed, key_weight, preferred_element_type=jnp.float32).astype(jnp.bfloat16)
    value_rows = jnp.dot(normed, value_weight, preferred_element_type=jnp.float32).astype(jnp.bfloat16)
    ratio = QH // KVH
    total = TOKENS
    key_pad = jnp.pad(key_rows, ((WIN, WIN), (0, 0)))
    value_pad = jnp.pad(value_rows, ((WIN, WIN), (0, 0)))
    sinks = sink_logit.reshape(KVH, ratio)

    def one_block(index):
        start = (index * TOK_DEV).astype(jnp.int32)
        query_block_tile = lax.dynamic_slice_in_dim(queries, start, TOK_DEV, 0).reshape(TOK_DEV, KVH, ratio, HEAD_SIZE)
        key_block_tile = lax.dynamic_slice_in_dim(key_pad, start, TOK_DEV + 2 * WIN, 0).reshape(-1, KVH, HEAD_SIZE)
        value_block_tile = lax.dynamic_slice_in_dim(value_pad, start, TOK_DEV + 2 * WIN, 0).reshape(-1, KVH, HEAD_SIZE)
        return attend_block(query_block_tile, key_block_tile, value_block_tile, start, sinks, total)
    attended = lax.map(one_block, jnp.arange(N_SP, dtype=jnp.int32)).reshape(TOKENS, QH * HEAD_SIZE)
    conv_gate = jnp.dot(normed, conv_gate_weight, preferred_element_type=jnp.float32).astype(jnp.bfloat16)
    conv_pre = jnp.dot(normed, conv_pre_weight, preferred_element_type=jnp.float32).astype(jnp.bfloat16)
    conv_input = jnp.dot(normed, conv_input_weight, preferred_element_type=jnp.float32).astype(jnp.bfloat16)
    product = (conv_pre.astype(jnp.float32) * conv_input.astype(jnp.float32)).astype(jnp.bfloat16)
    padded = jnp.pad(product.astype(jnp.float32), ((1, 1), (0, 0)))
    convolved = conv_taps[0] * padded[:-2] + conv_taps[1] * padded[1:-1] + conv_taps[2] * padded[2:]
    conv_out = (conv_gate.astype(jnp.float32) * convolved).astype(jnp.bfloat16)
    joined = jnp.concatenate([attended, conv_out], axis=1)
    return jnp.dot(joined, out_weight, preferred_element_type=jnp.float32).astype(jnp.bfloat16)
```

```python
import functools

import jax
import jax.numpy as jnp
from jax import lax
from jax.experimental import pallas as pl
from jax.experimental.pallas import tpu as pltpu
from jax.sharding import PartitionSpec as P


QH = 8
KVH = 4
HEAD_SIZE = 64
WIN = 128


def extended(block, sides, width):
    for axis, dim in sides:
        count = lax.axis_size(axis)
        forward = [(i, i + 1) for i in range(count - 1)]
        backward = [(target, source) for source, target in forward]
        low = lax.ppermute(
            lax.slice_in_dim(block, block.shape[dim] - width, None, axis=dim), axis, forward
        )
        high = lax.ppermute(lax.slice_in_dim(block, 0, width, axis=dim), axis, backward)
        block = jnp.concatenate([low, block, high], axis=dim)
    return block


def attend_local(query_block_tile, key_block_tile, value_block_tile, start, sinks, total):
    count = query_block_tile.shape[0]
    span = key_block_tile.shape[0]
    score_matrix = jnp.einsum(
        "yxpz,ixz->xpyi", query_block_tile, key_block_tile, preferred_element_type=jnp.float32
    ) * HEAD_SIZE ** (-0.5)
    query_pos = start + jnp.arange(count, dtype=jnp.int32)
    key_pos = start - WIN + jnp.arange(span, dtype=jnp.int32)
    valid = (
        (jnp.abs(query_pos[:, None] - key_pos[None, :]) <= WIN)
        & (key_pos[None, :] >= 0)
        & (key_pos[None, :] < total)
    )
    score_matrix = jnp.where(valid[None, None], score_matrix, -jnp.inf)
    sink_col = sinks[:, :, None, None]
    top = jnp.maximum(jnp.max(score_matrix, axis=-1, keepdims=True), sink_col)
    expo = jnp.exp(score_matrix - top)
    denom = jnp.sum(expo, axis=-1, keepdims=True) + jnp.exp(sink_col - top)
    weight_lower_precision = (expo / denom).astype(jnp.bfloat16)
    final_output = jnp.einsum(
        "bhcv,vbn->cbhn",
        weight_lower_precision,
        value_block_tile,
        preferred_element_type=jnp.float32,
    )
    return final_output.reshape(count, -1).astype(jnp.bfloat16)


def short_conv(conv_pad, conv_taps, conv_gate):
    count = conv_gate.shape[0]
    conv_f = conv_pad.astype(jnp.float32)
    convolved = (
        conv_taps[0] * conv_f[0:count]
        + conv_taps[1] * conv_f[1 : count + 1]
        + conv_taps[2] * conv_f[2 : count + 2]
    )
    return (conv_gate.astype(jnp.float32) * convolved).astype(jnp.bfloat16)


def body(
    tokens,
    norm_gain,
    query_weight,
    key_weight,
    value_weight,
    sink_logit,
    conv_gate_weight,
    conv_pre_weight,
    conv_input_weight,
    conv_taps,
    out_weight,
):
    tokens_f = tokens.astype(jnp.float32)
    normed = (
        tokens_f
        * lax.rsqrt(jnp.mean(tokens_f * tokens_f, axis=-1, keepdims=True) + 1e-06)
        * norm_gain
    ).astype(jnp.bfloat16)
    all_weight = jnp.concatenate(
        [
            query_weight,
            key_weight,
            value_weight,
            conv_gate_weight,
            conv_pre_weight,
            conv_input_weight,
        ],
        axis=1,
    )
    projected = jnp.dot(
        lax.all_gather(normed, "tp", axis=0, tiled=True),
        all_weight,
        preferred_element_type=jnp.float32,
    ).astype(jnp.bfloat16)
    query_width = query_weight.shape[1]
    kv_width = key_weight.shape[1]
    conv_width = conv_gate_weight.shape[1]
    edge_key = query_width + kv_width
    edge_value = edge_key + kv_width
    edge_gate = edge_value + conv_width
    edge_pre = edge_gate + conv_width
    queries = projected[:, :query_width]
    key_rows = projected[:, query_width:edge_key]
    value_rows = projected[:, edge_key:edge_value]
    conv_gate = projected[:, edge_value:edge_gate]
    conv_pre = projected[:, edge_gate:edge_pre]
    conv_input = projected[:, edge_pre:]
    product = (conv_pre.astype(jnp.float32) * conv_input.astype(jnp.float32)).astype(jnp.bfloat16)
    count = projected.shape[0]
    offset = lax.axis_index("sp") * count
    total = count * lax.axis_size("sp")
    padded = extended(jnp.concatenate([key_rows, value_rows, product], 1), (("sp", 0),), WIN)
    key_pad = padded[:, :kv_width]
    value_pad = padded[:, kv_width : 2 * kv_width]
    conv_pad = padded[WIN - 1 : WIN + count + 1, 2 * kv_width :]
    groups = kv_width // HEAD_SIZE
    ratio = QH // KVH
    query_block_tile = queries.reshape(count, groups, ratio, HEAD_SIZE)
    key_block_tile = key_pad.reshape(-1, groups, HEAD_SIZE)
    value_block_tile = value_pad.reshape(-1, groups, HEAD_SIZE)
    sinks = sink_logit.reshape(groups, ratio)
    conv_out = short_conv(conv_pad, conv_taps, conv_gate)
    attended = attend_local(
        query_block_tile, key_block_tile, value_block_tile, offset, sinks, total
    )
    attn_rows, conv_rows = (
        lax.all_to_all(attended, "tp", split_axis=0, concat_axis=1, tiled=True),
        lax.all_to_all(conv_out, "tp", split_axis=0, concat_axis=1, tiled=True),
    )
    joined = jnp.concatenate([attn_rows, conv_rows], axis=1)
    return jnp.dot(joined, out_weight, preferred_element_type=jnp.float32).astype(jnp.bfloat16)

EDGE = 16
ORDER = ("key", "value", "query", "gate", "pre", "input")
BF16 = jnp.bfloat16
F32 = jnp.float32


def gather_kernel(
    line,
    tokens,
    gain,
    w_key,
    w_value,
    w_query,
    w_gate,
    w_pre,
    w_input,
    small,
    q_out,
    kv_out,
    gate_out,
    prod_out,
    small_out,
    g_key,
    g_value,
    g_query,
    g_gate,
    g_pre,
    g_input,
    normed,
    edge_low,
    edge_high,
    pre_buf,
    send_sem,
    recv_sem,
    aux_send,
    aux_recv,
    local_sem,
):
    own = (w_key, w_value, w_query, w_gate, w_pre, w_input)
    got = (g_key, g_value, g_query, g_gate, g_pre, g_input)
    count = tokens.shape[0]
    depth = tokens.shape[1]
    s = lax.axis_index("sp")
    t = lax.axis_index("tp")
    other = 1 - t
    c = lax.rem(s, 2)
    y = lax.rem(s // 2, 2)
    z = s // 4
    n_sp = 4 * line
    chunks = n_sp
    rows = depth // chunks
    flat = 2 * s + t
    has_prev, has_next = flat > 0, flat < 2 * n_sp - 1
    prev = {"sp": jnp.maximum(flat - 1, 0) // 2, "tp": other}
    nxt = {"sp": jnp.minimum(flat + 1, 2 * n_sp - 1) // 2, "tp": other}
    has_left, has_right = z > 0, z < line - 1
    x_dev = {"sp": s, "tp": other}
    y_dev = {"sp": s + 2 - 4 * y, "tp": t}
    core_dev = {"sp": s + 1 - 2 * c, "tp": t}
    left_dev = {"sp": jnp.maximum(s - 4, lax.rem(s, 4)), "tp": t}
    right_dev = {"sp": jnp.minimum(s + 4, n_sp - 4 + lax.rem(s, 4)), "tp": t}

    def maybe(cond, fn):
        if cond is None:
            fn()
        else:
            pl.when(cond)(fn)

    barrier = pltpu.get_barrier_semaphore()
    greet = (
        (None, x_dev),
        (None, y_dev),
        (None, core_dev),
        (has_left, left_dev),
        (has_right, right_dev),
        (has_prev, prev),
        (has_next, nxt),
    )
    for cond, dev in greet:
        maybe(cond, lambda dev=dev: pl.semaphore_signal(barrier, inc=1, device_id=dev))
    peers = sum(1 if cond is None else cond.astype(jnp.int32) for cond, _ in greet)
    pl.semaphore_wait(barrier, peers)

    def chunk_of(core, yy, zz):
        return (core * 2 + yy) * line + zz

    def piece(ref, ch):
        return ref.at[pl.ds(pl.multiple_of(ch * rows, rows), rows), :]

    sends = []

    def send(cond, a, ch, dev, slot, first=False):
        copy = pltpu.make_async_remote_copy(
            src_ref=piece(own[a] if first else got[a], ch),
            dst_ref=piece(got[a], ch),
            send_sem=send_sem.at[a, slot],
            recv_sem=recv_sem.at[a, ch],
            device_id=dev,
        )
        maybe(cond, copy.start)
        sends.append((cond, copy))

    def arrived(cond, a, ch):
        part = piece(got[a], ch)
        maybe(cond, pltpu.make_async_copy(part, part, recv_sem.at[a, ch]).wait)

    aux = []

    def aux_copy(cond, src, dst, dev, slot, to_slot):
        copy = pltpu.make_async_remote_copy(
            src_ref=src,
            dst_ref=dst,
            send_sem=aux_send.at[slot],
            recv_sem=aux_recv.at[to_slot],
            device_id=dev,
        )
        maybe(cond, copy.start)
        aux.append((cond, copy))

    def aux_wait(cond, dst, slot):
        maybe(cond, pltpu.make_async_copy(dst, dst, aux_recv.at[slot]).wait)

    X0, X1, ZR, ZL, YS, CS = 0, 1, 2, 2 + line, 2 + 2 * line, 2 + 4 * line

    def x_sends(a):
        send(None, a, chunk_of(c, y, z), x_dev, X0, first=True)
        send(None, a, chunk_of(c, 1 - y, z), x_dev, X1, first=True)

    for a in range(2):
        x_sends(a)
    aux_copy(has_next, tokens.at[count - EDGE : count, :], edge_low, nxt, 0, 0)
    aux_copy(has_prev, tokens.at[0:EDGE, :], edge_high, prev, 1, 1)
    aux_copy(None, small, small_out.at[t], x_dev, 2, 2)
    for a in range(2, 6):
        x_sends(a)
    mine = pltpu.make_async_copy(small, small_out.at[t], local_sem.at[0])
    mine.start()

    def stage(a, d):
        if d == 0:
            arrived(None, a, chunk_of(c, y, z))
            send(has_right, a, chunk_of(c, y, z), right_dev, ZR)
            send(has_left, a, chunk_of(c, y, z), left_dev, ZL)
            send(None, a, chunk_of(c, y, z), core_dev, CS)
            arrived(None, a, chunk_of(c, 1 - y, z))
            send(None, a, chunk_of(c, 1 - y, z), core_dev, CS + 1)
            return
        if d < line:
            for side, (zz, here, onward, dev, slot) in enumerate(
                (
                    (z - d, z - d >= 0, has_right, right_dev, ZR + d),
                    (z + d, z + d < line, has_left, left_dev, ZL + d),
                )
            ):
                ch = chunk_of(c, y, jnp.clip(zz, 0, line - 1))
                arrived(here, a, ch)
                if d < line - 1:
                    send(here & onward, a, ch, dev, slot)
                send(here, a, ch, y_dev, YS + 2 * (d - 1) + side)
                send(here, a, ch, core_dev, CS + 2 * d + side)
        if d > 1:
            for side, (zz, here) in enumerate(((z - d + 1, z - d + 1 >= 0), (z + d - 1, z + d - 1 < line))):
                ch = chunk_of(c, 1 - y, jnp.clip(zz, 0, line - 1))
                arrived(here, a, ch)
                send(here, a, ch, core_dev, CS + 2 * (line + d - 2) + side)

    def complete(a):
        for i in range(2 * line):
            arrived(None, a, chunk_of(1 - c, 0, 0) + i)

    def norm(block):
        f = block.astype(F32)
        scale = lax.rsqrt(jnp.mean(f * f, axis=-1, keepdims=True) + 1e-06)
        return (f * scale * gain[...]).astype(BF16)

    def norm_main():
        def step(i, carry):
            r = pl.multiple_of(i * EDGE, EDGE)
            normed[pl.ds(r + EDGE, EDGE), :] = norm(tokens[pl.ds(r, EDGE), :])
            return carry

        lax.fori_loop(0, count // EDGE, step, 0, unroll=2)

    def norm_edges():
        aux_wait(has_prev, edge_low, 0)
        aux_wait(has_next, edge_high, 1)

        @pl.when(jnp.logical_not(has_prev))
        def _():
            edge_low[...] = jnp.zeros_like(edge_low)

        @pl.when(jnp.logical_not(has_next))
        def _():
            edge_high[...] = jnp.zeros_like(edge_high)

        normed[0:EDGE, :] = norm(edge_low[...])
        normed[count + EDGE :, :] = norm(edge_high[...])

    def lanes(ref, side, base=0):
        width = ref.shape[1]
        return pl.ds(pl.multiple_of(base + side * width, 128), width)

    def project(a, ref, side):
        kind = ORDER[a]
        if kind in ("pre", "input"):
            result = jnp.dot(normed[...], ref[...], preferred_element_type=F32).astype(BF16)
            if kind == "pre":
                pre_buf[:, lanes(ref, side)] = result
            else:
                cols = lanes(ref, side)
                prod_out[:, cols] = (
                    pre_buf[:, cols].astype(F32) * result.astype(F32)
                ).astype(BF16)
            return
        result = jnp.dot(
            normed[EDGE : EDGE + count, :], ref[...], preferred_element_type=F32
        ).astype(BF16)
        if kind == "query":
            q_out[:, lanes(ref, side)] = result
        elif kind == "gate":
            gate_out[:, lanes(ref, side)] = result
        else:
            base = 0 if kind == "key" else 2 * w_key.shape[1]
            kv_out[WIN : WIN + count, lanes(ref, side, base)] = result

    def send_halo():
        aux_copy(
            has_next, kv_out.at[count : count + WIN, :], kv_out.at[0:WIN, :], nxt, 3, 3
        )
        aux_copy(
            has_prev,
            kv_out.at[WIN : 2 * WIN, :],
            kv_out.at[count + WIN : count + 2 * WIN, :],
            prev,
            4,
            4,
        )

    norm_main()
    for wave in range(6 + line + 1):
        for d in range(line, -1, -1):
            if 0 <= wave - d < 6:
                stage(wave - d, d)
        if wave == 4:
            norm_edges()
        if wave < 6:
            project(wave, own[wave], t)
        done = wave - line - 1
        if 0 <= done < 6:
            complete(done)
            project(done, got[done], other)
            if done == 1:
                send_halo()

    @pl.when(jnp.logical_not(has_prev))
    def _():
        kv_out[0:WIN, :] = jnp.zeros((WIN, kv_out.shape[1]), BF16)

    @pl.when(jnp.logical_not(has_next))
    def _():
        kv_out[count + WIN :, :] = jnp.zeros((WIN, kv_out.shape[1]), BF16)

    aux_wait(None, small_out.at[other], 2)
    mine.wait()
    aux_wait(has_prev, kv_out.at[0:WIN, :], 3)
    aux_wait(has_next, kv_out.at[count + WIN : count + 2 * WIN, :], 4)
    for cond, copy in sends + aux:
        maybe(cond, copy.wait_send)


def mix_kernel(total, q_ref, kv_ref, gate_ref, prod_ref, small_ref, weight_ref, out_ref):
    count, heads_width = q_ref.shape[0], q_ref.shape[1]
    block = WIN
    step = pl.program_id(0)
    span = block + 2 * WIN
    start = (lax.axis_index("sp") * 2 + lax.axis_index("tp")) * (pl.num_programs(0) * block)
    start = start + step * block
    base = pl.multiple_of(step * block, block)
    row = lax.broadcasted_iota(jnp.int32, (block, span), 0)
    col = lax.broadcasted_iota(jnp.int32, (block, span), 1)
    key_pos = start - WIN + col
    valid = (col >= row) & (col - row <= 2 * WIN) & (key_pos >= 0) & (key_pos < total)
    kv_width = kv_ref.shape[1] // 2
    ratio = QH // KVH
    per_side = QH // 2
    pieces = []
    for h in range(QH):
        g = h // ratio
        q = q_ref[:, h * HEAD_SIZE : (h + 1) * HEAD_SIZE]
        k = kv_ref[pl.ds(base, span), g * HEAD_SIZE : (g + 1) * HEAD_SIZE]
        v = kv_ref[pl.ds(base, span), kv_width + g * HEAD_SIZE : kv_width + (g + 1) * HEAD_SIZE]
        scores = lax.dot_general(
            q, k, (((1,), (1,)), ((), ())), preferred_element_type=F32
        ) * HEAD_SIZE ** (-0.5)
        scores = jnp.where(valid, scores, -jnp.inf)
        i = h % per_side
        sink = small_ref[h // per_side, 3:4, i : i + 1]
        top = jnp.maximum(jnp.max(scores, axis=-1, keepdims=True), sink)
        expo = jnp.exp(scores - top)
        denom = jnp.sum(expo, axis=-1, keepdims=True) + jnp.exp(sink - top)
        weights = (expo * (1.0 / denom)).astype(BF16)
        pieces.append(jnp.dot(weights, v, preferred_element_type=F32).astype(BF16))
    attended = jnp.concatenate(pieces, axis=1)
    window = prod_ref[pl.ds(base, block + 2 * EDGE), :].astype(F32)
    taps = [
        jnp.concatenate([small_ref[0, j : j + 1, :], small_ref[1, j : j + 1, :]], axis=1)
        for j in range(3)
    ]
    convolved = (
        taps[0] * window[EDGE - 1 : EDGE - 1 + block]
        + taps[1] * window[EDGE : EDGE + block]
        + taps[2] * window[EDGE + 1 : EDGE + 1 + block]
    )
    conv_out = (gate_ref[...].astype(F32) * convolved).astype(BF16)
    joined = jnp.concatenate([attended, conv_out], axis=1)
    out_ref[...] = jnp.dot(joined, weight_ref[...], preferred_element_type=F32).astype(BF16)


def fast_body(
    line,
    tokens,
    norm_gain,
    query_weight,
    key_weight,
    value_weight,
    sink_logit,
    conv_gate_weight,
    conv_pre_weight,
    conv_input_weight,
    conv_taps,
    out_weight,
):
    count, depth = tokens.shape
    width = conv_taps.shape[1]
    small = jnp.concatenate(
        [
            conv_taps,
            jnp.pad(sink_logit[None, :], ((0, 0), (0, width - sink_logit.shape[0]))),
            jnp.zeros((4, width), F32),
        ],
        axis=0,
    )
    weights = (
        key_weight,
        value_weight,
        query_weight,
        conv_gate_weight,
        conv_pre_weight,
        conv_input_weight,
    )
    vmem = pl.BlockSpec(memory_space=pltpu.VMEM)
    kv_width = 2 * (key_weight.shape[1] + value_weight.shape[1])
    extended_rows = count + 2 * EDGE
    q, kv, gate, prod, small_all = pl.pallas_call(
        functools.partial(gather_kernel, line),
        out_shape=(
            jax.ShapeDtypeStruct((count, 2 * query_weight.shape[1]), BF16),
            jax.ShapeDtypeStruct((count + 2 * WIN, kv_width), BF16),
            jax.ShapeDtypeStruct((count, 2 * width), BF16),
            jax.ShapeDtypeStruct((extended_rows, 2 * width), BF16),
            jax.ShapeDtypeStruct((2, 8, width), F32),
        ),
        in_specs=[vmem] * 9,
        out_specs=(vmem,) * 5,
        scratch_shapes=[pltpu.VMEM(w.shape, BF16) for w in weights]
        + [
            pltpu.VMEM((extended_rows, depth), BF16),
            pltpu.VMEM((EDGE, depth), BF16),
            pltpu.VMEM((EDGE, depth), BF16),
            pltpu.VMEM((extended_rows, 2 * width), BF16),
            pltpu.SemaphoreType.DMA((6, 2 + 8 * line)),
            pltpu.SemaphoreType.DMA((6, 4 * line)),
            pltpu.SemaphoreType.DMA((5,)),
            pltpu.SemaphoreType.DMA((5,)),
            pltpu.SemaphoreType.DMA((1,)),
        ],
        compiler_params=pltpu.CompilerParams(
            collective_id=0, has_side_effects=True, vmem_limit_bytes=40 * 2**20
        ),
    )(tokens, norm_gain.reshape(1, depth), *weights, small)
    blocks = count // WIN
    whole = lambda a: pl.BlockSpec(a.shape, lambda i: (0,) * a.ndim)
    tile = lambda a: pl.BlockSpec((WIN, a.shape[1]), lambda i: (i, 0))
    return pl.pallas_call(
        functools.partial(mix_kernel, count * 8 * line),
        grid=(blocks,),
        out_shape=jax.ShapeDtypeStruct((count, out_weight.shape[1]), BF16),
        in_specs=[tile(q), whole(kv), tile(gate), whole(prod), whole(small_all), whole(out_weight)],
        out_specs=pl.BlockSpec((WIN, out_weight.shape[1]), lambda i: (i, 0)),
        compiler_params=pltpu.CompilerParams(vmem_limit_bytes=40 * 2**20),
    )(q, kv, gate, prod, small_all, out_weight)


def solution(mesh):
    placed = (
        P(("sp", "tp"), None),
        P(),
        P(None, "tp"),
        P(None, "tp"),
        P(None, "tp"),
        P("tp"),
        P(None, "tp"),
        P(None, "tp"),
        P(None, "tp"),
        P(None, "tp"),
        P(),
    )
    n_sp, n_tp = mesh.shape["sp"], mesh.shape["tp"]
    line = n_sp // 4
    paired = n_tp == 2 and n_sp % 4 == 0 and line >= 2
    chosen = functools.partial(fast_body, line) if paired else body
    return jax.shard_map(
        chosen, mesh=mesh, in_specs=placed, out_specs=P(("sp", "tp"), None), check_vma=False
    )
```

```python
import functools

import jax
import jax.numpy as jnp
from jax import lax
from jax.experimental import pallas as pl
from jax.experimental.pallas import tpu as pltpu
from jax.sharding import PartitionSpec as P


QH = 8
KVH = 4
HEAD_SIZE = 64
WIN = 128


def extended(block, sides, width):
    for axis, dim in sides:
        count = lax.axis_size(axis)
        forward = [(i, i + 1) for i in range(count - 1)]
        backward = [(target, source) for source, target in forward]
        low = lax.ppermute(
            lax.slice_in_dim(block, block.shape[dim] - width, None, axis=dim), axis, forward
        )
        high = lax.ppermute(lax.slice_in_dim(block, 0, width, axis=dim), axis, backward)
        block = jnp.concatenate([low, block, high], axis=dim)
    return block


def attend_local(query_block_tile, key_block_tile, value_block_tile, start, sinks, total):
    count = query_block_tile.shape[0]
    span = key_block_tile.shape[0]
    score_matrix = jnp.einsum(
        "yxpz,ixz->xpyi", query_block_tile, key_block_tile, preferred_element_type=jnp.float32
    ) * HEAD_SIZE ** (-0.5)
    query_pos = start + jnp.arange(count, dtype=jnp.int32)
    key_pos = start - WIN + jnp.arange(span, dtype=jnp.int32)
    valid = (
        (jnp.abs(query_pos[:, None] - key_pos[None, :]) <= WIN)
        & (key_pos[None, :] >= 0)
        & (key_pos[None, :] < total)
    )
    score_matrix = jnp.where(valid[None, None], score_matrix, -jnp.inf)
    sink_col = sinks[:, :, None, None]
    top = jnp.maximum(jnp.max(score_matrix, axis=-1, keepdims=True), sink_col)
    expo = jnp.exp(score_matrix - top)
    denom = jnp.sum(expo, axis=-1, keepdims=True) + jnp.exp(sink_col - top)
    weight_lower_precision = (expo / denom).astype(jnp.bfloat16)
    final_output = jnp.einsum(
        "bhcv,vbn->cbhn",
        weight_lower_precision,
        value_block_tile,
        preferred_element_type=jnp.float32,
    )
    return final_output.reshape(count, -1).astype(jnp.bfloat16)


def short_conv(conv_pad, conv_taps, conv_gate):
    count = conv_gate.shape[0]
    conv_f = conv_pad.astype(jnp.float32)
    convolved = (
        conv_taps[0] * conv_f[0:count]
        + conv_taps[1] * conv_f[1 : count + 1]
        + conv_taps[2] * conv_f[2 : count + 2]
    )
    return (conv_gate.astype(jnp.float32) * convolved).astype(jnp.bfloat16)


def body(
    tokens,
    norm_gain,
    query_weight,
    key_weight,
    value_weight,
    sink_logit,
    conv_gate_weight,
    conv_pre_weight,
    conv_input_weight,
    conv_taps,
    out_weight,
):
    tokens_f = tokens.astype(jnp.float32)
    normed = (
        tokens_f
        * lax.rsqrt(jnp.mean(tokens_f * tokens_f, axis=-1, keepdims=True) + 1e-06)
        * norm_gain
    ).astype(jnp.bfloat16)
    all_weight = jnp.concatenate(
        [
            query_weight,
            key_weight,
            value_weight,
            conv_gate_weight,
            conv_pre_weight,
            conv_input_weight,
        ],
        axis=1,
    )
    projected = jnp.dot(
        lax.all_gather(normed, "tp", axis=0, tiled=True),
        all_weight,
        preferred_element_type=jnp.float32,
    ).astype(jnp.bfloat16)
    query_width = query_weight.shape[1]
    kv_width = key_weight.shape[1]
    conv_width = conv_gate_weight.shape[1]
    edge_key = query_width + kv_width
    edge_value = edge_key + kv_width
    edge_gate = edge_value + conv_width
    edge_pre = edge_gate + conv_width
    queries = projected[:, :query_width]
    key_rows = projected[:, query_width:edge_key]
    value_rows = projected[:, edge_key:edge_value]
    conv_gate = projected[:, edge_value:edge_gate]
    conv_pre = projected[:, edge_gate:edge_pre]
    conv_input = projected[:, edge_pre:]
    product = (conv_pre.astype(jnp.float32) * conv_input.astype(jnp.float32)).astype(jnp.bfloat16)
    count = projected.shape[0]
    offset = lax.axis_index("sp") * count
    total = count * lax.axis_size("sp")
    padded = extended(jnp.concatenate([key_rows, value_rows, product], 1), (("sp", 0),), WIN)
    key_pad = padded[:, :kv_width]
    value_pad = padded[:, kv_width : 2 * kv_width]
    conv_pad = padded[WIN - 1 : WIN + count + 1, 2 * kv_width :]
    groups = kv_width // HEAD_SIZE
    ratio = QH // KVH
    query_block_tile = queries.reshape(count, groups, ratio, HEAD_SIZE)
    key_block_tile = key_pad.reshape(-1, groups, HEAD_SIZE)
    value_block_tile = value_pad.reshape(-1, groups, HEAD_SIZE)
    sinks = sink_logit.reshape(groups, ratio)
    conv_out = short_conv(conv_pad, conv_taps, conv_gate)
    attended = attend_local(
        query_block_tile, key_block_tile, value_block_tile, offset, sinks, total
    )
    attn_rows, conv_rows = (
        lax.all_to_all(attended, "tp", split_axis=0, concat_axis=1, tiled=True),
        lax.all_to_all(conv_out, "tp", split_axis=0, concat_axis=1, tiled=True),
    )
    joined = jnp.concatenate([attn_rows, conv_rows], axis=1)
    return jnp.dot(joined, out_weight, preferred_element_type=jnp.float32).astype(jnp.bfloat16)

EDGE = 16
ORDER = ("key", "value", "query", "gate", "pre", "input")
BF16 = jnp.bfloat16
F32 = jnp.float32


def gather_kernel(
    line,
    tokens_hbm,
    gain,
    h_key,
    h_value,
    h_query,
    h_gate,
    h_pre,
    h_input,
    small,
    out_hbm,
    result_ref,
    tokens,
    w_key,
    w_value,
    w_query,
    w_gate,
    w_pre,
    w_input,
    out_weight,
    q_out,
    kv_out,
    gate_out,
    prod_out,
    small_out,
    attended,
    partial,
    g_key,
    g_value,
    g_query,
    g_gate,
    g_pre,
    g_input,
    normed,
    edge_low,
    edge_high,
    pre_buf,
    send_sem,
    recv_sem,
    aux_send,
    aux_recv,
    local_sem,
):
    held = (h_key, h_value, h_query, h_gate, h_pre, h_input)
    own = (w_key, w_value, w_query, w_gate, w_pre, w_input)
    got = (g_key, g_value, g_query, g_gate, g_pre, g_input)
    count = tokens.shape[0]
    depth = tokens.shape[1]
    s = lax.axis_index("sp")
    t = lax.axis_index("tp")
    other = 1 - t
    c = lax.rem(s, 2)
    y = lax.rem(s // 2, 2)
    z = s // 4
    n_sp = 4 * line
    chunks = n_sp
    rows = depth // chunks
    flat = 2 * s + t
    has_prev, has_next = flat > 0, flat < 2 * n_sp - 1
    prev = {"sp": jnp.maximum(flat - 1, 0) // 2, "tp": other}
    nxt = {"sp": jnp.minimum(flat + 1, 2 * n_sp - 1) // 2, "tp": other}
    has_left, has_right = z > 0, z < line - 1
    x_dev = {"sp": s, "tp": other}
    y_dev = {"sp": s + 2 - 4 * y, "tp": t}
    core_dev = {"sp": s + 1 - 2 * c, "tp": t}
    left_dev = {"sp": jnp.maximum(s - 4, lax.rem(s, 4)), "tp": t}
    right_dev = {"sp": jnp.minimum(s + 4, n_sp - 4 + lax.rem(s, 4)), "tp": t}

    def maybe(cond, fn):
        if cond is None:
            fn()
        else:
            pl.when(cond)(fn)

    load_tokens = pltpu.make_async_copy(tokens_hbm, tokens, local_sem.at[1])
    load_tokens.start()
    load_out = pltpu.make_async_copy(out_hbm, out_weight, local_sem.at[2])
    loads = [pltpu.make_async_copy(held[a], own[a], local_sem.at[3 + a]) for a in range(6)]

    barrier = pltpu.get_barrier_semaphore()
    greet = (
        (None, x_dev),
        (None, y_dev),
        (None, core_dev),
        (has_left, left_dev),
        (has_right, right_dev),
        (has_prev, prev),
        (has_next, nxt),
    )
    for cond, dev in greet:
        maybe(cond, lambda dev=dev: pl.semaphore_signal(barrier, inc=1, device_id=dev))
    peers = sum(1 if cond is None else cond.astype(jnp.int32) for cond, _ in greet)
    pl.semaphore_wait(barrier, peers)

    def chunk_of(core, yy, zz):
        return (core * 2 + yy) * line + zz

    def piece(ref, ch):
        return ref.at[pl.ds(pl.multiple_of(ch * rows, rows), rows), :]

    sends = []

    def send(cond, a, ch, dev, slot, first=False):
        copy = pltpu.make_async_remote_copy(
            src_ref=piece(held[a] if first else got[a], ch),
            dst_ref=piece(got[a], ch),
            send_sem=send_sem.at[a, slot],
            recv_sem=recv_sem.at[a, ch],
            device_id=dev,
        )
        maybe(cond, copy.start)
        sends.append((cond, copy))

    def arrived(cond, a, ch):
        part = piece(got[a], ch)
        maybe(cond, pltpu.make_async_copy(part, part, recv_sem.at[a, ch]).wait)

    aux = []

    def aux_copy(cond, src, dst, dev, slot, to_slot):
        copy = pltpu.make_async_remote_copy(
            src_ref=src,
            dst_ref=dst,
            send_sem=aux_send.at[slot],
            recv_sem=aux_recv.at[to_slot],
            device_id=dev,
        )
        maybe(cond, copy.start)
        aux.append((cond, copy))

    def aux_wait(cond, dst, slot):
        maybe(cond, pltpu.make_async_copy(dst, dst, aux_recv.at[slot]).wait)

    X0, X1, ZR, ZL, YS, CS = 0, 1, 2, 2 + line, 2 + 2 * line, 2 + 4 * line

    def x_sends(a):
        send(None, a, chunk_of(c, y, z), x_dev, X0, first=True)
        send(None, a, chunk_of(c, 1 - y, z), x_dev, X1, first=True)

    for a in range(2):
        x_sends(a)
    aux_copy(has_next, tokens_hbm.at[count - EDGE : count, :], edge_low, nxt, 0, 0)
    aux_copy(has_prev, tokens_hbm.at[0:EDGE, :], edge_high, prev, 1, 1)
    aux_copy(None, small, small_out.at[t], x_dev, 2, 2)
    for a in range(2, 6):
        x_sends(a)
    mine = pltpu.make_async_copy(small, small_out.at[t], local_sem.at[0])
    mine.start()

    def stage(a, d):
        if d == 0:
            arrived(None, a, chunk_of(c, y, z))
            send(has_right, a, chunk_of(c, y, z), right_dev, ZR)
            send(has_left, a, chunk_of(c, y, z), left_dev, ZL)
            send(None, a, chunk_of(c, y, z), core_dev, CS)
            arrived(None, a, chunk_of(c, 1 - y, z))
            send(None, a, chunk_of(c, 1 - y, z), core_dev, CS + 1)
            return
        if d < line:
            for side, (zz, here, onward, dev, slot) in enumerate(
                (
                    (z - d, z - d >= 0, has_right, right_dev, ZR + d),
                    (z + d, z + d < line, has_left, left_dev, ZL + d),
                )
            ):
                ch = chunk_of(c, y, jnp.clip(zz, 0, line - 1))
                arrived(here, a, ch)
                if d < line - 1:
                    send(here & onward, a, ch, dev, slot)
                send(here, a, ch, y_dev, YS + 2 * (d - 1) + side)
                send(here, a, ch, core_dev, CS + 2 * d + side)
        if d > 1:
            for side, (zz, here) in enumerate(((z - d + 1, z - d + 1 >= 0), (z + d - 1, z + d - 1 < line))):
                ch = chunk_of(c, 1 - y, jnp.clip(zz, 0, line - 1))
                arrived(here, a, ch)
                send(here, a, ch, core_dev, CS + 2 * (line + d - 2) + side)

    def complete(a):
        for i in range(2 * line):
            arrived(None, a, chunk_of(1 - c, 0, 0) + i)

    def norm(block):
        f = block.astype(F32)
        scale = lax.rsqrt(jnp.mean(f * f, axis=-1, keepdims=True) + 1e-06)
        return (f * scale * gain[...]).astype(BF16)

    def norm_main():
        def step(i, carry):
            r = pl.multiple_of(i * EDGE, EDGE)
            normed[pl.ds(r + EDGE, EDGE), :] = norm(tokens[pl.ds(r, EDGE), :])
            return carry

        lax.fori_loop(0, count // EDGE, step, 0, unroll=2)

    def norm_edges():
        aux_wait(has_prev, edge_low, 0)
        aux_wait(has_next, edge_high, 1)

        @pl.when(jnp.logical_not(has_prev))
        def _():
            edge_low[...] = jnp.zeros_like(edge_low)

        @pl.when(jnp.logical_not(has_next))
        def _():
            edge_high[...] = jnp.zeros_like(edge_high)

        normed[0:EDGE, :] = norm(edge_low[...])
        normed[count + EDGE :, :] = norm(edge_high[...])

    def lanes(ref, side, base=0):
        width = ref.shape[1]
        return pl.ds(pl.multiple_of(base + side * width, 128), width)

    def project(a, ref, side):
        kind = ORDER[a]
        if kind in ("pre", "input"):
            result = jnp.dot(normed[...], ref[...], preferred_element_type=F32).astype(BF16)
            if kind == "pre":
                pre_buf[:, lanes(ref, side)] = result
            else:
                cols = lanes(ref, side)
                prod_out[:, cols] = (
                    pre_buf[:, cols].astype(F32) * result.astype(F32)
                ).astype(BF16)
            return
        result = jnp.dot(
            normed[EDGE : EDGE + count, :], ref[...], preferred_element_type=F32
        ).astype(BF16)
        if kind == "query":
            q_out[:, lanes(ref, side)] = result
        elif kind == "gate":
            gate_out[:, lanes(ref, side)] = result
        else:
            base = 0 if kind == "key" else 2 * w_key.shape[1]
            kv_out[WIN : WIN + count, lanes(ref, side, base)] = result

    def send_halo():
        aux_copy(
            has_next, kv_out.at[count : count + WIN, :], kv_out.at[0:WIN, :], nxt, 3, 3
        )
        aux_copy(
            has_prev,
            kv_out.at[WIN : 2 * WIN, :],
            kv_out.at[count + WIN : count + 2 * WIN, :],
            prev,
            4,
            4,
        )

    def attend(b):
        span = 3 * WIN
        base = b * WIN
        row = lax.broadcasted_iota(jnp.int32, (WIN, span), 0)
        col = lax.broadcasted_iota(jnp.int32, (WIN, span), 1)
        key_pos = flat * count + base - WIN + col
        valid = (
            (col >= row)
            & (col - row <= 2 * WIN)
            & (key_pos >= 0)
            & (key_pos < 2 * n_sp * count)
        )
        kv_width = kv_out.shape[1] // 2
        ratio = QH // KVH
        per_side = QH // 2
        for g in range(KVH):
            k = kv_out[base : base + span, g * HEAD_SIZE : (g + 1) * HEAD_SIZE]
            v = kv_out[
                base : base + span,
                kv_width + g * HEAD_SIZE : kv_width + (g + 1) * HEAD_SIZE,
            ]
            parts = []
            for h in range(g * ratio, (g + 1) * ratio):
                q = q_out[base : base + WIN, h * HEAD_SIZE : (h + 1) * HEAD_SIZE]
                scores = lax.dot_general(
                    q, k, (((1,), (1,)), ((), ())), preferred_element_type=F32
                ) * HEAD_SIZE ** (-0.5)
                scores = jnp.where(valid, scores, -jnp.inf)
                i = h % per_side
                sink = small_out[h // per_side, 3:4, i : i + 1]
                top = jnp.maximum(jnp.max(scores, axis=-1, keepdims=True), sink)
                expo = jnp.exp(scores - top)
                denom = jnp.sum(expo, axis=-1, keepdims=True) + jnp.exp(sink - top)
                weights = (expo * (1.0 / denom)).astype(BF16)
                parts.append(jnp.dot(weights, v, preferred_element_type=F32).astype(BF16))
            width = ratio * HEAD_SIZE
            attended[base : base + WIN, g * width : (g + 1) * width] = jnp.concatenate(
                parts, axis=1
            )

    def before_attention():
        @pl.when(jnp.logical_not(has_prev))
        def _():
            kv_out[0:WIN, :] = jnp.zeros((WIN, kv_out.shape[1]), BF16)

        @pl.when(jnp.logical_not(has_next))
        def _():
            kv_out[count + WIN :, :] = jnp.zeros((WIN, kv_out.shape[1]), BF16)

        aux_wait(None, small_out.at[other], 2)
        mine.wait()
        aux_wait(has_prev, kv_out.at[0:WIN, :], 3)
        aux_wait(has_next, kv_out.at[count + WIN : count + 2 * WIN, :], 4)

    def finish():
        half = attended.shape[1]
        taps = [
            jnp.concatenate([small_out[0, j : j + 1, :], small_out[1, j : j + 1, :]], axis=1)
            for j in range(3)
        ]
        for b in range(count // WIN):
            base = b * WIN
            window = prod_out[base : base + WIN + 2 * EDGE, :].astype(F32)
            convolved = (
                taps[0] * window[EDGE - 1 : EDGE - 1 + WIN]
                + taps[1] * window[EDGE : EDGE + WIN]
                + taps[2] * window[EDGE + 1 : EDGE + 1 + WIN]
            )
            conv_out = (gate_out[base : base + WIN, :].astype(F32) * convolved).astype(BF16)
            result_ref[base : base + WIN, :] = (
                partial[base : base + WIN, :]
                + jnp.dot(conv_out, out_weight[half:, :], preferred_element_type=F32)
            ).astype(BF16)

    for load in loads:
        load.start()
    load_out.start()
    load_tokens.wait()
    norm_main()
    lag = 2
    blocks = count // WIN
    last = 5 + lag * line
    for wave in range(last + 1):
        for d in range(line, -1, -1):
            if 0 <= wave - lag * d < 6:
                stage(wave - lag * d, d)
        if wave == 4:
            norm_edges()
        if wave < 6:
            loads[wave].wait()
            project(wave, own[wave], t)
        done = wave - lag * line
        if 0 <= done < 6:
            if done == 3:
                before_attention()
                attend(0)
            if done == 4:
                for b in range(1, blocks):
                    attend(b)
            if done == 5:
                load_out.wait()
                partial[...] = jnp.dot(
                    attended[...],
                    out_weight[: attended.shape[1], :],
                    preferred_element_type=F32,
                )
            complete(done)
            project(done, got[done], other)
            if done == 1:
                send_halo()
    finish()
    for cond, copy in sends + aux:
        maybe(cond, copy.wait_send)


def fast_body(
    line,
    tokens,
    norm_gain,
    query_weight,
    key_weight,
    value_weight,
    sink_logit,
    conv_gate_weight,
    conv_pre_weight,
    conv_input_weight,
    conv_taps,
    out_weight,
):
    count, depth = tokens.shape
    width = conv_taps.shape[1]
    small = jnp.concatenate(
        [
            conv_taps,
            jnp.pad(sink_logit[None, :], ((0, 0), (0, width - sink_logit.shape[0]))),
            jnp.zeros((4, width), F32),
        ],
        axis=0,
    )
    weights = (
        key_weight,
        value_weight,
        query_weight,
        conv_gate_weight,
        conv_pre_weight,
        conv_input_weight,
    )
    vmem = pl.BlockSpec(memory_space=pltpu.VMEM)
    hbm = pl.BlockSpec(memory_space=pltpu.HBM)
    kv_width = 2 * (key_weight.shape[1] + value_weight.shape[1])
    heads_width = 2 * query_weight.shape[1]
    extended_rows = count + 2 * EDGE
    return pl.pallas_call(
        functools.partial(gather_kernel, line),
        out_shape=jax.ShapeDtypeStruct((count, out_weight.shape[1]), BF16),
        in_specs=[hbm, vmem] + [hbm] * 6 + [vmem, hbm],
        out_specs=vmem,
        scratch_shapes=[pltpu.VMEM((count, depth), BF16)]
        + [pltpu.VMEM(w.shape, BF16) for w in weights]
        + [
            pltpu.VMEM(out_weight.shape, BF16),
            pltpu.VMEM((count, heads_width), BF16),
            pltpu.VMEM((count + 2 * WIN, kv_width), BF16),
            pltpu.VMEM((count, 2 * width), BF16),
            pltpu.VMEM((extended_rows, 2 * width), BF16),
            pltpu.VMEM((2, 8, width), F32),
            pltpu.VMEM((count, heads_width), BF16),
            pltpu.VMEM((count, out_weight.shape[1]), F32),
        ]
        + [pltpu.VMEM(w.shape, BF16) for w in weights]
        + [
            pltpu.VMEM((extended_rows, depth), BF16),
            pltpu.VMEM((EDGE, depth), BF16),
            pltpu.VMEM((EDGE, depth), BF16),
            pltpu.VMEM((extended_rows, 2 * width), BF16),
            pltpu.SemaphoreType.DMA((6, 2 + 8 * line)),
            pltpu.SemaphoreType.DMA((6, 4 * line)),
            pltpu.SemaphoreType.DMA((5,)),
            pltpu.SemaphoreType.DMA((5,)),
            pltpu.SemaphoreType.DMA((9,)),
        ],
        compiler_params=pltpu.CompilerParams(
            collective_id=0, has_side_effects=True, vmem_limit_bytes=58 * 2**20
        ),
    )(tokens, norm_gain.reshape(1, depth), *weights, small, out_weight)


def solution(mesh):
    placed = (
        P(("sp", "tp"), None),
        P(),
        P(None, "tp"),
        P(None, "tp"),
        P(None, "tp"),
        P("tp"),
        P(None, "tp"),
        P(None, "tp"),
        P(None, "tp"),
        P(None, "tp"),
        P(),
    )
    n_sp, n_tp = mesh.shape["sp"], mesh.shape["tp"]
    line = n_sp // 4
    paired = n_tp == 2 and n_sp % 4 == 0 and line >= 2
    chosen = functools.partial(fast_body, line) if paired else body
    return jax.shard_map(
        chosen, mesh=mesh, in_specs=placed, out_specs=P(("sp", "tp"), None), check_vma=False
    )
```
